32 devices in a mesh: ep: 8 (over z, y), tp: 4 (over x, core).
Axes of the slice: x: 2, y: 2, z: 4, core: 2. Of those that a mesh axis runs over, the one named last changes fastest.
Arguments:
- query_rows: bfloat16 [16384, 1024], P('ep', 'tp'), may hold values from -6 to 6
- key_rows: bfloat16 [16384, 1024], P('ep', 'tp'), may hold values from -6 to 6
- value_rows: bfloat16 [16384, 2048], P('ep', 'tp'), may hold values from -6 to 6
- gate_rows: bfloat16 [16384, 2048], P('ep', 'tp'), may hold values from -6 to 6
- log_decay: float32 [8, 16384], P('tp', 'ep'), may hold values from -1 to 0
- out_proj: bfloat16 [2048, 2048], P('tp'), may hold values from -0.125 to 0.125
- moe_input: bfloat16 [4096, 2048], P(('ep', 'tp')), may hold values from -6 to 6
- norm_gain: float32 [2048], replicated, may hold values from 0.1 to 1.9
- routing: int32 [4096, 4], P(('ep', 'tp')), may hold values from 0 to 31, all different within a row; in each aligned block of 128 rows (0 to 127, 128 to 255, ...) at most 32 rows name the same one
- route_weight: float32 [4096, 4], P(('ep', 'tp')), may hold values from 0.2 to 1
- expert_gate: bfloat16 [32, 2048, 512], P(('ep', 'tp')), may hold values from -0.125 to 0.125
- expert_up: bfloat16 [32, 2048, 512], P(('ep', 'tp')), may hold values from -0.125 to 0.125
- expert_down: bfloat16 [32, 512, 2048], P(('ep', 'tp')), may hold values from -0.25 to 0.25
- shared_gate: bfloat16 [2048, 512], replicated, may hold values from -0.125 to 0.125
- shared_up: bfloat16 [2048, 512], replicated, may hold values from -0.125 to 0.125
- shared_down: bfloat16 [512, 2048], replicated, may hold values from -0.25 to 0.25
Outputs:
- mixer_out: bfloat16 [16384, 2048], P(('ep', 'tp'))
- moe_out: bfloat16 [4096, 2048], P(('ep', 'tp'))
The draws below stay inside these ranges and needn't reach their ends.
Inputs may be any that keep to these rules, and one draw needn't show every extreme that they name: `routing`: within the rows of one device no expert is named more than 32 times.
All inputs are finite; a program needn't handle non-finite values.
Results may differ from the reference program's by a relative error of at most 0.019.
Values may be sent and summed in bfloat16 or wider, within the bound.
A program may use at most 128 MiB of HBM per device.

```python
import math
import jax
import jax.numpy as jnp
import numpy as np
from jax import lax

D = 2048
RETENTION_HEADS = 8
DK = 128
DV = 256
BLOCK = 128
TOK_A = 2048
TOKENS_A = 16384
FF = 512
SHARED_FF = 512
TOP = 4
TOK_B = 128
TOKENS_B = 4096
EXPERTS = 32
CAP = 32
N_EP = 8
N_TP = 4


def draw_log_decay(key, part):
    random_subkeys = jax.random.split(jax.random.fold_in(key, 17), 7)
    sequence_length = TOKENS_A
    fast_share = 0.5
    quick_decay_mask = jax.random.uniform(random_subkeys[0], (RETENTION_HEADS,)) < fast_share
    fast_rate = jnp.log(10.0) / jax.random.uniform(random_subkeys[1], (RETENTION_HEADS,), minval=30.0, maxval=100.0)
    slow_rate = jax.random.uniform(random_subkeys[2], (RETENTION_HEADS,), minval=0.2, maxval=0.6) / sequence_length
    base_rate = jnp.where(quick_decay_mask, fast_rate, slow_rate)
    position_index = jnp.arange(sequence_length)
    span_factor = jnp.exp(jax.random.uniform(random_subkeys[3], (sequence_length // TOK_A,), minval=-0.7, maxval=0.7))
    jitter = jnp.exp(jax.random.uniform(random_subkeys[4], (RETENTION_HEADS, sequence_length), minval=-0.35, maxval=0.35))
    chosen_places = jax.random.randint(random_subkeys[5], (3,), 0, sequence_length)
    spike_selected = jnp.any(position_index[None, :] == chosen_places[:, None], axis=0)
    spike_dropped = jnp.log(jax.random.uniform(random_subkeys[6], (RETENTION_HEADS, sequence_length), minval=0.5, maxval=0.8))
    smoothed_decay = -base_rate[:, None] * span_factor[position_index // TOK_A][None, :] * jitter
    selected_mask = spike_selected[None, :] & jnp.logical_not(quick_decay_mask)[:, None]
    return jnp.where(selected_mask, smoothed_decay + spike_dropped, smoothed_decay).astype(jnp.float32)


def steps_of(rng, shape, cuts, smallest, top_value):
    def one(dim, shards_of):
        steps = jax.random.uniform(jax.random.fold_in(jax.random.fold_in(rng, 6), dim), (shards_of,), jnp.float32, smallest / len(cuts), top_value / len(cuts))
        return jnp.repeat(jnp.exp(steps), shape[dim] // shards_of).reshape((-1,) + (1,) * (len(shape) - dim - 1))

    loudness = one(*cuts[0])
    for cut in cuts[1:]:
        loudness = loudness * one(*cut)
    return loudness


def deal_out(rng, own, number, rows, count, top, limit, skew):
    sequence = jax.random.permutation(rng, count)
    crowded, common = portions_of(count, rows * top, limit, skew, True), portions_of(count, rows * top, limit, skew, False)
    places = jnp.arange(count)

    def named(tallies, rotation):
        used = int((tallies > 0).sum())
        fixed = max(1, used // 4)
        passed = fixed + (places - fixed + rotation * (used - fixed)) % max(1, count - fixed)
        return jnp.zeros((count,), jnp.int32).at[sequence[jnp.where(places < fixed, places, passed)]].set(jnp.asarray(tallies, jnp.int32))

    tallies = jnp.where(number % 4 == 0, named(crowded, number // 4), named(common, number - number // 4 - 1))
    mixed = jax.random.permutation(jax.random.fold_in(own, 3), count)
    giver, taker = mixed[0:count // 2 * 2:2], mixed[1:count // 2 * 2:2]
    margin = jnp.minimum(tallies[giver] - 1, limit - tallies[taker]) // 2
    margin = jnp.where((giver == sequence[0]) | (taker == sequence[0]) | (tallies[taker] == 0), 0, jnp.maximum(margin, 0))
    passed = jax.random.randint(jax.random.fold_in(own, 4), (count // 2,), 0, 1 << 20) % (margin + 1)
    tallies = tallies.at[giver].add(-passed).at[taker].add(passed)
    items = jnp.searchsorted(jnp.cumsum(tallies), jnp.arange(rows * top), side="right").astype(jnp.int32)
    listing = items.reshape(top, rows).T
    listing = listing[jax.random.permutation(jax.random.fold_in(own, 1), rows)]
    rotation = jax.random.randint(jax.random.fold_in(own, 2), (rows, 1), 0, top)
    return jnp.take_along_axis(listing, (jnp.arange(top)[None, :] + rotation) % top, axis=1)


def portions_of(number_of, total, most, skew, full):
    portions = [(1 << 20) // math.isqrt(rank ** skew) + 1 for rank in range(1, number_of + 1)]
    largest = most if full else min(most, max(-(-total // number_of), total * portions[0] // sum(portions)))
    least = 1 if total - largest >= number_of - 1 else 0
    given, spare = [largest] + [least] * (number_of - 1), total - largest - least * (number_of - 1)
    while spare > 0:
        candidates = [i for i in range(1, number_of) if given[i] < largest] or [i for i in range(1, number_of) if given[i] < most]
        whole, budget = sum([portions[i] for i in candidates]), spare
        for i in candidates:
            more = min(most - given[i], max(1, budget * portions[i] // whole), spare)
            given[i] = given[i] + more
            spare = spare - more
    return np.array(given)


def bell_draw(rng, shape, width, reach, pieces=(), held_as=jnp.bfloat16):
    loudness = steps_of(rng, shape, pieces, -0.22, 0.18) if pieces else 1.0
    entries = jax.random.normal(rng, shape, jnp.float32) * width * loudness
    return jnp.minimum(jnp.maximum(entries, -reach), reach).astype(held_as)


def setup_inputs(seed: int = 0) -> dict:
    keys = jax.random.split(jax.random.key(seed), 17)
    query_rows = bell_draw(keys[0], (TOKENS_A, RETENTION_HEADS * DK), 1.0, 6.0, ((0, 8), (1, 4)))
    key_rows = bell_draw(keys[1], (TOKENS_A, RETENTION_HEADS * DK), 1.0, 6.0, ((0, 8), (1, 4)))
    value_rows = bell_draw(keys[2], (TOKENS_A, RETENTION_HEADS * DV), 1.0, 6.0, ((0, 8), (1, 4)))
    gate_rows = bell_draw(keys[3], (TOKENS_A, RETENTION_HEADS * DV), 1.0, 6.0, ((0, 8), (1, 4)))
    log_decay = draw_log_decay(jax.random.fold_in(keys[16], 71), 0)
    out_proj = bell_draw(keys[5], (RETENTION_HEADS * DV, D), (RETENTION_HEADS * DV) ** -0.5, 0.125, ((0, 4),))
    moe_input = bell_draw(keys[6], (TOKENS_B, D), 1.0, 6.0, ((0, 32),))
    norm_gain = jnp.clip(1.0 + 0.18 * jax.random.normal(keys[7], (D,), jnp.float32), 0.1, 1.9)
    routing_keys = jax.random.split(jax.random.fold_in(keys[8], 1), TOKENS_B // TOK_B)
    routing_turns = jax.random.permutation(jax.random.fold_in(keys[8], 3), TOKENS_B // TOK_B)
    routing = jax.vmap(lambda own, number: deal_out(jax.random.fold_in(keys[8], 2), own, number, TOK_B, EXPERTS, TOP, CAP, 2))(routing_keys, routing_turns).reshape((TOKENS_B, TOP))
    route_weight = jnp.clip(0.2 + 0.8 * jax.random.uniform(keys[9], (TOKENS_B, TOP), jnp.float32) ** steps_of(keys[9], (TOKENS_B, TOP), ((0, 32),), -0.2, 0.2), 0.2, 1.0)
    expert_gate = bell_draw(keys[10], (EXPERTS, D, FF), D ** -0.5, 0.125, ((0, 32),))
    expert_up = bell_draw(keys[11], (EXPERTS, D, FF), D ** -0.5, 0.125, ((0, 32),))
    expert_down = bell_draw(keys[12], (EXPERTS, FF, D), FF ** -0.5, 0.25, ((0, 32),))
    shared_gate = bell_draw(keys[13], (D, SHARED_FF), D ** -0.5, 0.125)
    shared_up = bell_draw(keys[14], (D, SHARED_FF), D ** -0.5, 0.125)
    shared_down = bell_draw(keys[15], (SHARED_FF, D), SHARED_FF ** -0.5, 0.25)
    return {"query_rows": query_rows, "key_rows": key_rows, "value_rows": value_rows, "gate_rows": gate_rows, "log_decay": log_decay, "out_proj": out_proj, "moe_input": moe_input, "norm_gain": norm_gain, "routing": routing, "route_weight": route_weight, "expert_gate": expert_gate, "expert_up": expert_up, "expert_down": expert_down, "shared_gate": shared_gate, "shared_up": shared_up, "shared_down": shared_down}


EPS = 1e-06

def retention_all(query_rows, key_rows, value_rows, log_decay):
    n_blocks = TOKENS_A // BLOCK
    score_scale = DK ** (-0.5)
    q_blocks = query_rows.reshape(n_blocks, BLOCK, RETENTION_HEADS, DK)
    k_blocks = key_rows.reshape(n_blocks, BLOCK, RETENTION_HEADS, DK)
    v_blocks = value_rows.reshape(n_blocks, BLOCK, RETENTION_HEADS, DV)
    a_blocks = jnp.transpose(log_decay.reshape(RETENTION_HEADS, n_blocks, BLOCK), (1, 0, 2))
    causal = jnp.arange(BLOCK)[:, None] >= jnp.arange(BLOCK)[None, :]

    def advance(carried_state, block_in):
        q_blk, k_blk, v_blk, a_blk = block_in
        cum_decay = jnp.cumsum(a_blk, axis=1)
        block_count = cum_decay[:, -1]
        query_float = q_blk.astype(jnp.float32)
        key_float = k_blk.astype(jnp.float32)
        value_float = v_blk.astype(jnp.float32)
        retention_scores = jnp.einsum('gab,lab->agl', query_float, key_float)
        log_gap = jnp.where(causal[None], cum_decay[:, :, None] - cum_decay[:, None, :], 0.0)
        decay_mat = jnp.where(causal[None], jnp.exp(log_gap), 0.0)
        weight = (retention_scores * score_scale * decay_mat).astype(jnp.bfloat16)
        weight = lax.optimization_barrier(weight).astype(jnp.float32)
        inner_out = jnp.einsum('hnm,mhe->nhe', weight, value_float)
        state_low = lax.optimization_barrier(carried_state.astype(jnp.bfloat16)).astype(jnp.float32)
        cross_out = jnp.einsum('nhd,hde->nhe', query_float, state_low) * jnp.exp(cum_decay).T[:, :, None]
        decayed_key_rows = (key_float * score_scale * jnp.exp(block_count[None, :] - cum_decay.T)[:, :, None]).astype(jnp.bfloat16)
        decayed_key_rows = lax.optimization_barrier(decayed_key_rows).astype(jnp.float32)
        carried_state = carried_state * jnp.exp(block_count)[:, None, None] + jnp.einsum('czq,czy->zqy', decayed_key_rows, value_float)
        return (carried_state, inner_out + cross_out)
    initial = jnp.zeros((RETENTION_HEADS, DK, DV), jnp.float32)
    _, outputs = lax.scan(advance, initial, (q_blocks, k_blocks, v_blocks, a_blocks))
    return outputs.reshape(TOKENS_A, RETENTION_HEADS, DV)

def expert_apply(inputs, w_gate, w_up, w_down):
    gate_act = jnp.dot(inputs, w_gate, preferred_element_type=jnp.float32)
    up_act = jnp.dot(inputs, w_up, preferred_element_type=jnp.float32)
    hidden = (jax.nn.silu(gate_act) * up_act).astype(jnp.bfloat16)
    return jnp.dot(hidden, w_down, preferred_element_type=jnp.float32)

def reference(query_rows, key_rows, value_rows, gate_rows, log_decay, out_proj, moe_input, norm_gain, routing, route_weight, expert_gate, expert_up, expert_down, shared_gate, shared_up, shared_down):
    raw_out = retention_all(query_rows, key_rows, value_rows, log_decay)
    avg_out = lax.optimization_barrier(jnp.mean(raw_out, axis=-1, keepdims=True))
    spread = lax.optimization_barrier(jnp.mean(jnp.square(raw_out - avg_out), axis=-1, keepdims=True))
    normed = (raw_out - avg_out) * lax.rsqrt(spread + EPS)
    gate_act = jax.nn.silu(gate_rows.astype(jnp.float32).reshape(TOKENS_A, RETENTION_HEADS, DV))
    retained = (gate_act * normed).reshape(TOKENS_A, RETENTION_HEADS * DV).astype(jnp.bfloat16)
    group_cols = RETENTION_HEADS * DV // N_TP
    summed = jnp.zeros((TOKENS_A, D), jnp.float32)
    for group_idx in range(N_TP):
        lo_col = group_idx * group_cols
        partial_sum = jnp.dot(retained[:, lo_col:lo_col + group_cols], out_proj[lo_col:lo_col + group_cols], preferred_element_type=jnp.float32).astype(jnp.bfloat16)
        summed = summed + partial_sum.astype(jnp.float32)
    mixer_out = summed.astype(jnp.bfloat16)
    as_float = moe_input.astype(jnp.float32)
    moe_normed = (as_float * lax.rsqrt(lax.optimization_barrier(jnp.mean(as_float * as_float, axis=-1, keepdims=True)) + EPS) * norm_gain).astype(jnp.bfloat16)
    flat_route = routing.reshape(-1)
    flat_weight = route_weight.reshape(-1)
    bound_rows = N_EP * N_TP * CAP

    def visit(total_out, expert_idx):
        picked_rows = jnp.nonzero(flat_route == expert_idx, size=bound_rows, fill_value=0)[0].astype(jnp.int32)
        live_mask = (jnp.arange(bound_rows) < jnp.sum((flat_route == expert_idx).astype(jnp.int32))).astype(jnp.float32)
        token_idx = picked_rows // TOP
        result = expert_apply(moe_normed[token_idx], expert_gate[expert_idx], expert_up[expert_idx], expert_down[expert_idx])
        result = lax.optimization_barrier(result.astype(jnp.bfloat16)).astype(jnp.float32)
        scaled = result * (flat_weight[picked_rows] * live_mask)[:, None]
        return (total_out.at[token_idx].add(scaled), None)
    routed, _ = lax.scan(visit, jnp.zeros((TOKENS_B, D), jnp.float32), jnp.arange(N_EP * N_TP, dtype=jnp.int32))
    shared = expert_apply(moe_normed, shared_gate, shared_up, shared_down)
    moe_out = (routed + shared).astype(jnp.bfloat16)
    return (mixer_out, moe_out)
```

```python
import functools
import math

import jax
import jax.numpy as jnp
from jax import lax
from jax.experimental import pallas as pl
from jax.experimental.pallas import tpu as pltpu
from jax.sharding import PartitionSpec as P

DK = 128
DV = 256
BLOCK = 128
EPS = 1e-06
Z_GROUPS = 4

F32 = jnp.float32
BF16 = jnp.bfloat16
MESH = pl.DeviceIdType.MESH


def dot(a, b):
    return jnp.dot(a, b, preferred_element_type=F32)


def silu(v):
    return v / (1.0 + jnp.exp(-v))


def kernel(
    E, T, G, C,
    x_ref, gain_ref, meta_ref, cum_ref, cumc_ref, tot_ref,
    q_hbm, k_hbm, v_hbm, g_hbm, op_hbm,
    wg_hbm, wu_hbm, wd_hbm, sg_hbm, su_hbm, sd_hbm,
    mix_ref, moe_ref,
    q_v, k_v, v_v, g_v, op_v, wg_v, wu_v, wd_v,
    xz, mz, dsp, rcv, ret, dwt, shr, prcv,
    upd, sblk, lend, srcv, trcv, rs, rr, inc,
    load_sem,
    z_s, z_r, m_s, m_r, d_s, d_r, b_s, b_r, p_s, p_r, s_s, s_r, t_s, t_r, o_s, o_r, r_s, r_r,
):
    ep = lax.axis_index("ep")
    tp = lax.axis_index("tp")
    R = E // G
    Pn = R * T
    zi = ep // R
    yi = ep % R
    j = yi * T + tp
    tok, width = x_ref.shape
    n_visits = meta_ref.shape[0] // 2
    nb = cum_ref.shape[0]
    H = cum_ref.shape[1]
    nbc = nb // T
    scale = DK ** (-0.5)

    loads = [
        pltpu.make_async_copy(src, dst, load_sem.at[i])
        for i, (src, dst) in enumerate(
            ((k_hbm, k_v), (v_hbm, v_v), (op_hbm, op_v.at[0]), (sg_hbm, wg_v), (su_hbm, wu_v),
             (sd_hbm, wd_v), (q_hbm, q_v), (g_hbm, g_v), (wg_hbm.at[0], wg_v),
             (wu_hbm.at[0], wu_v), (wd_hbm.at[0], wd_v))
        )
    ]
    for c in loads[:8]:
        c.start()

    def z_peer(r):
        return (((zi + r) % G) * R + yi, tp)

    def plane_peer(d):
        p = (j + d) % Pn
        return (zi * R + p // T, p % T)

    def tp_peer(i):
        return (ep, (tp + i) % T)

    barrier = pltpu.get_barrier_semaphore()

    @pl.loop(1, Pn)
    def _(d):
        pl.semaphore_signal(barrier, inc=1, device_id=plane_peer(d), device_id_type=MESH)

    @pl.loop(1, E)
    def _(d):
        pl.semaphore_signal(barrier, inc=1, device_id=((ep + d) % E, tp), device_id_type=MESH)

    xf = x_ref[...].astype(F32)
    xz[0] = (
        xf * lax.rsqrt(jnp.mean(xf * xf, axis=-1, keepdims=True) + EPS) * gain_ref[...]
    ).astype(BF16)
    mz[0] = meta_ref[...]
    pl.semaphore_wait(barrier, Pn - 1 + E - 1)

    def rcopy(src, dst, ss, rs_, dev):
        return pltpu.make_async_remote_copy(
            src_ref=src, dst_ref=dst, send_sem=ss, recv_sem=rs_, device_id=dev, device_id_type=MESH
        )

    def z_copy(r):
        return rcopy(xz.at[0], xz.at[r], z_s.at[r], z_r.at[r], z_peer(r))

    def m_copy(r):
        return rcopy(mz.at[0], mz.at[r], m_s.at[r], m_r.at[r], z_peer(r))

    def rows(d):
        return pl.ds(pl.multiple_of(d * C, C), C)

    def d_copy(r, d):
        return rcopy(dsp.at[r, rows(d)], rcv.at[r, rows(d)], d_s.at[r, d], d_r.at[r, d],
                     plane_peer(d))

    def b_copy(r, d):
        return rcopy(rcv.at[r, rows(d)], ret.at[r, rows(d)], b_s.at[r, d], b_r.at[r, d],
                     plane_peer(Pn - d))

    def p_copy(r):
        return rcopy(dsp.at[r, 0:tok], prcv.at[r - 1], p_s.at[r], p_r.at[r], z_peer(G - r))

    def s_copy(d):
        return rcopy(lend, srcv.at[d - 1], s_s.at[d], s_r.at[d], ((ep + d) % E, tp))

    def t_copy(d):
        return rcopy(tot_ref, trcv.at[d], t_s.at[d], t_r.at[d], ((ep + d) % E, tp))

    def o_copy(i):
        return rcopy(op_v.at[0], op_v.at[i], o_s.at[i], o_r.at[i], tp_peer(i))

    def r_copy(i):
        return rcopy(rs.at[i], rr.at[i - 1], r_s.at[i], r_r.at[i], tp_peer(i))

    @pl.loop(1, G)
    def _(r):
        m_copy(r).start()
        z_copy(r).start()

    def dispatch(r):
        meta = mz[r]
        owner = lax.broadcasted_iota(jnp.int32, (Pn, tok), 0)
        owner = (zi * Pn + (owner + j) % Pn).astype(F32)
        member = jnp.zeros((Pn, tok), F32)
        weight = jnp.zeros((Pn, tok), F32)
        for v in range(n_visits):
            hit = meta[v:v + 1, :] == owner
            member += jnp.where(hit, 1.0, 0.0)
            weight += jnp.where(hit, meta[n_visits + v:n_visits + v + 1, :], 0.0)
        before = lax.broadcasted_iota(jnp.int32, (tok, tok), 0) < lax.broadcasted_iota(
            jnp.int32, (tok, tok), 1
        )
        rank = dot(member.astype(BF16), jnp.where(before, 1.0, 0.0).astype(BF16))
        rank = jnp.where(member > 0.5, rank, -1.0)
        slot = lax.broadcasted_iota(jnp.int32, (C, tok), 0).astype(F32)
        picks, wts = [], []
        for d in range(Pn):
            eq = slot == rank[d:d + 1, :]
            picks.append(jnp.where(eq, 1.0, 0.0))
            wts.append(jnp.where(eq, weight[d:d + 1, :], 0.0))
        pick = jnp.concatenate(picks, axis=0).astype(BF16)
        dwt[r] = jnp.concatenate(wts, axis=0).T.astype(BF16)
        out = dot(pick, xz[r]).astype(BF16)
        dsp[r] = out
        rcv[r, 0:C] = out[0:C]

        @pl.loop(1, Pn)
        def _(d):
            d_copy(r, d).start()

    dispatch(0)

    loads[0].wait()
    loads[1].wait()

    inc[...] = jnp.zeros_like(inc)

    @pl.loop(0, nb)
    def _(b):
        rb = pl.ds(pl.multiple_of(b * BLOCK, BLOCK), BLOCK)
        cumc = cumc_ref[b]
        crow = cum_ref[b]
        for h in range(H):
            col = cumc[:, h:h + 1]
            last = crow[h:h + 1, BLOCK - 1:BLOCK]
            u = (k_v[rb, h * DK:(h + 1) * DK].astype(F32) * (scale * jnp.exp(last - col))).astype(BF16)
            add = lax.dot_general(
                u, v_v[rb, h * DV:(h + 1) * DV], (((0,), (0,)), ((), ())),
                preferred_element_type=F32,
            )
            upd[b, h] = add
            inc[h] = inc[h] * jnp.exp(last) + add

    lend[...] = inc[...].astype(BF16)

    @pl.loop(1, E)
    def _(d):
        @pl.when(ep + d < E)
        def _():
            t_copy(d).start()
            s_copy(d).start()

    @pl.loop(1, G)
    def _(r):
        m_copy(r).wait_recv()
        z_copy(r).wait_recv()
        dispatch(r)

    loads[2].wait()

    @pl.loop(1, T)
    def _(i):
        o_copy(i).start()

    loads[3].wait()
    loads[4].wait()
    loads[5].wait()
    hid = (silu(dot(xz[0], wg_v[...])) * dot(xz[0], wu_v[...])).astype(BF16)
    shr[...] = dot(hid, wd_v[...])
    for c in loads[8:]:
        c.start()

    inc[...] = jnp.zeros_like(inc)

    @pl.loop(1, E)
    def _(i):
        d = E - i

        @pl.when(ep >= d)
        def _():
            t_copy(d).wait_recv()
            s_copy(d).wait_recv()
            for h in range(H):
                shrink = jnp.exp(trcv[d, h:h + 1, 0:1])
                inc[h] = inc[h] * shrink + srcv[d - 1, h].astype(F32)

    @pl.loop(0, nb)
    def _(b):
        crow = cum_ref[b]
        for h in range(H):
            s = inc[h]
            sblk[b, h] = s.astype(BF16)
            inc[h] = s * jnp.exp(crow[h:h + 1, BLOCK - 1:BLOCK]) + upd[b, h]

    loads[6].wait()
    loads[7].wait()
    causal = lax.broadcasted_iota(jnp.int32, (BLOCK, BLOCK), 0) >= lax.broadcasted_iota(
        jnp.int32, (BLOCK, BLOCK), 1
    )

    def retain(i):
        chunk = (tp + i) % T

        @pl.loop(0, nbc)
        def _(w):
            b = chunk * nbc + w
            rb = pl.ds(pl.multiple_of(b * BLOCK, BLOCK), BLOCK)
            ro = pl.ds(pl.multiple_of(w * BLOCK, BLOCK), BLOCK)
            cumc = cumc_ref[b]
            crow = cum_ref[b]
            for h in range(H):
                col = cumc[:, h:h + 1]
                row = crow[h:h + 1, :]
                qb = q_v[rb, h * DK:(h + 1) * DK]
                kb = k_v[rb, h * DK:(h + 1) * DK]
                vb = v_v[rb, h * DV:(h + 1) * DV]
                sc = lax.dot_general(qb, kb, (((1,), (1,)), ((), ())), preferred_element_type=F32)
                dec = jnp.exp(jnp.where(causal, col - row, 0.0))
                wt = jnp.where(causal, sc * scale * dec, 0.0).astype(BF16)
                raw = dot(wt, vb) + dot(qb, sblk[b, h]) * jnp.exp(col)
                avg = jnp.mean(raw, axis=-1, keepdims=True)
                cen = raw - avg
                var = jnp.mean(cen * cen, axis=-1, keepdims=True)
                gate = g_v[rb, h * DV:(h + 1) * DV].astype(F32)
                rs[i, ro, h * DV:(h + 1) * DV] = (
                    silu(gate) * (cen * lax.rsqrt(var + EPS))
                ).astype(BF16)

    @pl.loop(1, T)
    def _(i):
        retain(i)
        r_copy(i).start()

    retain(0)

    loads[8].wait()
    loads[9].wait()
    loads[10].wait()

    @pl.loop(0, G)
    def _(r):
        @pl.loop(1, Pn)
        def _(d):
            d_copy(r, d).wait_recv()

        rows_in = rcv[r]
        hidden = (silu(dot(rows_in, wg_v[...])) * dot(rows_in, wu_v[...])).astype(BF16)
        res = dot(hidden, wd_v[...]).astype(BF16)
        rcv[r] = res
        ret[r, 0:C] = res[0:C]

        @pl.loop(1, Pn)
        def _(d):
            b_copy(r, d).start()

    @pl.loop(1, G)
    def _(r):
        @pl.loop(1, Pn)
        def _(d):
            b_copy(r, d).wait_recv()

        @pl.loop(1, Pn)
        def _(d):
            d_copy(r, d).wait_send()

        dsp[r, 0:tok] = dot(dwt[r], ret[r]).astype(BF16)
        p_copy(r).start()

    @pl.loop(1, T)
    def _(i):
        o_copy(i).wait_recv()
        r_copy(i).wait_recv()

    n_col = 512
    @pl.loop(0, width // n_col)
    def _(n):
        cols = pl.ds(pl.multiple_of(n * n_col, n_col), n_col)
        acc = dot(rs[0], op_v[0, :, cols])
        for i in range(1, T):
            acc += dot(rr[i - 1], op_v[i, :, cols])
        mix_ref[:, cols] = acc.astype(BF16)

    @pl.loop(1, Pn)
    def _(d):
        b_copy(0, d).wait_recv()

    total = dot(dwt[0], ret[0]) + shr[...]
    for r in range(1, G):
        p_copy(r).wait_recv()
        total += prcv[r - 1].astype(F32)
    moe_ref[...] = total.astype(BF16)

    @pl.loop(1, G)
    def _(r):
        m_copy(r).wait_send()
        z_copy(r).wait_send()
        p_copy(r).wait_send()

    @pl.loop(0, G)
    def _(r):
        @pl.loop(1, Pn)
        def _(d):
            b_copy(r, d).wait_send()

    @pl.loop(1, Pn)
    def _(d):
        d_copy(0, d).wait_send()

    @pl.loop(1, E)
    def _(d):
        @pl.when(ep + d < E)
        def _():
            t_copy(d).wait_send()
            s_copy(d).wait_send()

    @pl.loop(1, T)
    def _(i):
        o_copy(i).wait_send()
        r_copy(i).wait_send()


def local(
    query_rows, key_rows, value_rows, gate_rows, log_decay, out_proj,
    moe_input, norm_gain, routing, route_weight,
    expert_gate, expert_up, expert_down, shared_gate, shared_up, shared_down,
):
    E, T = lax.axis_size("ep"), lax.axis_size("tp")
    G = math.gcd(E, Z_GROUPS)
    Pn = (E // G) * T
    n = query_rows.shape[0]
    H = query_rows.shape[1] // DK
    nb = n // BLOCK
    tok, width = moe_input.shape
    visits = routing.shape[1]
    C = 2 * tok * visits // (E * T)
    ff = expert_gate.shape[2]
    assert shared_gate.shape[1] == ff
    rows_o = n // T
    dvl = H * DV

    cum = jnp.cumsum(log_decay.reshape(H, nb, BLOCK), axis=2)
    tot = jnp.sum(cum[:, :, -1], axis=1)
    tot = jnp.broadcast_to(jnp.pad(tot, (0, -H % 8))[:, None], (H + (-H % 8), 128))
    cum_b = cum.transpose(1, 0, 2)
    cum_c = cum.transpose(1, 2, 0)
    meta = jnp.concatenate([routing.T.astype(F32), route_weight.T], axis=0)

    vm = pl.BlockSpec(memory_space=pltpu.VMEM)
    hb = pl.BlockSpec(memory_space=pl.ANY)
    V = pltpu.VMEM
    dma = pltpu.SemaphoreType.DMA
    scratch = [
        V((n, H * DK), BF16), V((n, H * DK), BF16), V((n, dvl), BF16), V((n, dvl), BF16),
        V((T,) + out_proj.shape, BF16),
        V((width, ff), BF16), V((width, ff), BF16), V((ff, width), BF16),
        V((G, tok, width), BF16), V((G, 2 * visits, tok), F32),
        V((G, Pn * C, width), BF16), V((G, Pn * C, width), BF16), V((G, Pn * C, width), BF16),
        V((G, tok, Pn * C), BF16), V((tok, width), F32), V((G - 1, tok, width), BF16),
        V((nb, H, DK, DV), F32), V((nb, H, DK, DV), BF16), V((H, DK, DV), BF16),
        V((E - 1, H, DK, DV), BF16), V((E,) + tot.shape, F32),
        V((T, rows_o, dvl), BF16), V((T - 1, rows_o, dvl), BF16), V((H, DK, DV), F32),
        dma((11,)),
        dma((G,)), dma((G,)), dma((G,)), dma((G,)),
        dma((G, Pn)), dma((G, Pn)), dma((G, Pn)), dma((G, Pn)),
        dma((G,)), dma((G,)),
        dma((E,)), dma((E,)), dma((E,)), dma((E,)),
        dma((T,)), dma((T,)), dma((T,)), dma((T,)),
    ]
    return pl.pallas_call(
        functools.partial(kernel, E, T, G, C),
        out_shape=(
            jax.ShapeDtypeStruct((rows_o, width), BF16),
            jax.ShapeDtypeStruct((tok, width), BF16),
        ),
        in_specs=[vm] * 6 + [hb] * 11,
        out_specs=(vm, vm),
        scratch_shapes=scratch,
        compiler_params=pltpu.CompilerParams(
            collective_id=0, has_side_effects=True, vmem_limit_bytes=67043328
        ),
        name="fused",
    )(
        moe_input, norm_gain[None, :], meta, cum_b, cum_c, tot,
        query_rows, key_rows, value_rows, gate_rows, out_proj,
        expert_gate, expert_up, expert_down, shared_gate, shared_up, shared_down,
    )


def solution(mesh):
    both = P(("ep", "tp"), None)
    in_specs = (
        P("ep", "tp"), P("ep", "tp"), P("ep", "tp"), P("ep", "tp"), P("tp", "ep"), P("tp", None),
        both, P(), both, both,
        P(("ep", "tp"), None, None), P(("ep", "tp"), None, None), P(("ep", "tp"), None, None),
        P(), P(), P(),
    )
    return jax.shard_map(
        local, mesh=mesh, in_specs=in_specs, out_specs=(both, both), check_vma=False
    )
```

```python
import functools
import math

import jax
import jax.numpy as jnp
from jax import lax
from jax.experimental import pallas as pl
from jax.experimental.pallas import tpu as pltpu
from jax.sharding import PartitionSpec as P

DK = 128
DV = 256
BLOCK = 128
EPS = 1e-06
Z_GROUPS = 4

F32 = jnp.float32
BF16 = jnp.bfloat16
MESH = pl.DeviceIdType.MESH


def dot(a, b):
    return jnp.dot(a, b, preferred_element_type=F32)


def silu(v):
    return v / (1.0 + jnp.exp(-v))


def kernel(
    E, T, G, C,
    x_ref, gain_ref, meta_ref, cum_ref, cumc_ref, tot_ref,
    q_hbm, k_hbm, v_hbm, g_hbm, op_hbm,
    wg_hbm, wu_hbm, wd_hbm, sg_hbm, su_hbm, sd_hbm,
    mix_ref, moe_ref,
    q_v, k_v, v_v, g_v, op_v, wg_v, wu_v, wd_v,
    xz, mz, dsp, rcv, ret, dwt, shr, prcv,
    upd, sblk, lend, srcv, trcv, rs, rr, inc,
    load_sem,
    z_s, z_r, m_s, m_r, d_s, d_r, b_s, b_r, p_s, p_r, s_s, s_r, t_s, t_r,
    o1_s, o1_r, o2_s, o2_r, o3_s, o3_r, r_s, r_r,
):
    ep = lax.axis_index("ep")
    tp = lax.axis_index("tp")
    R = E // G
    Pn = R * T
    zi = ep // R
    yi = ep % R
    j = yi * T + tp
    tok, width = x_ref.shape
    n_visits = meta_ref.shape[0] // 2
    nb = cum_ref.shape[0]
    H = cum_ref.shape[1]
    nbc = nb // T
    B = math.gcd(T, 2)
    A = T // B
    ta, tb = tp // B, tp % B
    piece = op_v.shape[1] // R
    scale = DK ** (-0.5)

    loads = [
        pltpu.make_async_copy(src, dst, load_sem.at[i])
        for i, (src, dst) in enumerate(
            ((k_hbm, k_v), (v_hbm, v_v), (op_hbm, op_v.at[tp]), (sg_hbm, wg_v), (su_hbm, wu_v),
             (sd_hbm, wd_v), (q_hbm, q_v), (g_hbm, g_v), (wg_hbm.at[0], wg_v),
             (wu_hbm.at[0], wu_v), (wd_hbm.at[0], wd_v))
        )
    ]
    for c in loads[:8]:
        c.start()

    def z_place(g):
        return (g * R + yi, tp)

    def plane_peer(d):
        p = (j + d) % Pn
        return (zi * R + p // T, p % T)

    def tp_peer(i):
        return (ep, (tp + i) % T)

    barrier = pltpu.get_barrier_semaphore()

    @pl.loop(1, Pn)
    def _(d):
        pl.semaphore_signal(barrier, inc=1, device_id=plane_peer(d), device_id_type=MESH)

    @pl.loop(1, E)
    def _(d):
        pl.semaphore_signal(barrier, inc=1, device_id=((ep + d) % E, tp), device_id_type=MESH)

    xf = x_ref[...].astype(F32)
    xz[zi] = (
        xf * lax.rsqrt(jnp.mean(xf * xf, axis=-1, keepdims=True) + EPS) * gain_ref[...]
    ).astype(BF16)
    mz[zi] = meta_ref[...]
    pl.semaphore_wait(barrier, Pn - 1 + E - 1)

    def rcopy(src, dst, ss, rs_, dev):
        return pltpu.make_async_remote_copy(
            src_ref=src, dst_ref=dst, send_sem=ss, recv_sem=rs_, device_id=dev, device_id_type=MESH
        )

    def z_copy(g, way):
        to = (zi - 1, zi + 1)[way]
        return rcopy(xz.at[g], xz.at[g], z_s.at[way, g], z_r.at[g], z_place(to))

    def m_copy(g, way):
        to = (zi - 1, zi + 1)[way]
        return rcopy(mz.at[g], mz.at[g], m_s.at[way, g], m_r.at[g], z_place(to))

    def z_sends(g, way):
        if way:
            return (g <= zi) & (zi + 1 < G)
        return (g >= zi) & (zi > 0)

    def group_at(i):
        dist = (i + 1) // 2
        g = zi + jnp.where(i % 2 == 1, -dist, dist)
        return g, (g >= 0) & (g < G)

    def rows(d):
        return pl.ds(pl.multiple_of(d * C, C), C)

    def d_copy(r, d):
        return rcopy(dsp.at[r, rows(d)], rcv.at[r, rows(d)], d_s.at[r, d], d_r.at[r, d],
                     plane_peer(d))

    def b_copy(r, d):
        return rcopy(rcv.at[r, rows(d)], ret.at[r, rows(d)], b_s.at[r, d], b_r.at[r, d],
                     plane_peer(Pn - d))

    def p_copy(g):
        return rcopy(dsp.at[g, 0:tok], prcv.at[zi], p_s.at[g], p_r.at[zi], z_place(g))

    def p_arrival(g):
        return rcopy(dsp.at[g, 0:tok], prcv.at[g], p_s.at[g], p_r.at[g], z_place(g))

    def s_copy(d):
        return rcopy(lend, srcv.at[d - 1], s_s.at[d], s_r.at[d], ((ep + d) % E, tp))

    def t_copy(d):
        return rcopy(tot_ref, trcv.at[d], t_s.at[d], t_r.at[d], ((ep + d) % E, tp))

    def shard(da, db=0):
        return ((ta + A - da) % A) * B + (tb + B - db) % B

    def part(y):
        return pl.ds(pl.multiple_of(y * piece, piece), piece)

    def o1_copy(da, src):
        at = op_v.at[src, part(yi)]
        return rcopy(at, at, o1_s.at[da], o1_r.at[da], (ep, ((ta + da) % A) * B + tb))

    def o2_copy(da, dy, y):
        at = op_v.at[shard(da), part(y)]
        return rcopy(at, at, o2_s.at[da, dy], o2_r.at[da, dy], (zi * R + (yi + dy) % R, tp))

    def o3_copy(da, db, src):
        at = op_v.at[src]
        return rcopy(at, at, o3_s.at[da, db], o3_r.at[da, db], (ep, ta * B + (tb + db) % B))

    def r_copy(i):
        return rcopy(rs.at[i], rr.at[i - 1], r_s.at[i], r_r.at[i], tp_peer(i))

    for way in (0, 1):
        @pl.when(z_sends(zi, way))
        def _():
            m_copy(zi, way).start()
            z_copy(zi, way).start()

    def dispatch(r):
        meta = mz[r]
        owner = lax.broadcasted_iota(jnp.int32, (Pn, tok), 0)
        owner = (zi * Pn + (owner + j) % Pn).astype(F32)
        member = jnp.zeros((Pn, tok), F32)
        weight = jnp.zeros((Pn, tok), F32)
        for v in range(n_visits):
            hit = meta[v:v + 1, :] == owner
            member += jnp.where(hit, 1.0, 0.0)
            weight += jnp.where(hit, meta[n_visits + v:n_visits + v + 1, :], 0.0)
        before = lax.broadcasted_iota(jnp.int32, (tok, tok), 0) < lax.broadcasted_iota(
            jnp.int32, (tok, tok), 1
        )
        rank = dot(member.astype(BF16), jnp.where(before, 1.0, 0.0).astype(BF16))
        rank = jnp.where(member > 0.5, rank, -1.0)
        slot = lax.broadcasted_iota(jnp.int32, (C, tok), 0).astype(F32)
        picks, wts = [], []
        for d in range(Pn):
            eq = slot == rank[d:d + 1, :]
            picks.append(jnp.where(eq, 1.0, 0.0))
            wts.append(jnp.where(eq, weight[d:d + 1, :], 0.0))
        pick = jnp.concatenate(picks, axis=0).astype(BF16)
        dwt[r] = jnp.concatenate(wts, axis=0).T.astype(BF16)
        out = dot(pick, xz[r]).astype(BF16)
        dsp[r] = out
        rcv[r, 0:C] = out[0:C]

        @pl.loop(1, Pn)
        def _(d):
            d_copy(r, d).start()

    dispatch(zi)
    loads[2].wait()
    for da in range(1, A):
        o1_copy(da, tp).start()

    loads[0].wait()
    loads[1].wait()

    inc[...] = jnp.zeros_like(inc)

    @pl.loop(0, nb)
    def _(b):
        rb = pl.ds(pl.multiple_of(b * BLOCK, BLOCK), BLOCK)
        cumc = cumc_ref[b]
        crow = cum_ref[b]
        for h in range(H):
            col = cumc[:, h:h + 1]
            last = crow[h:h + 1, BLOCK - 1:BLOCK]
            u = (k_v[rb, h * DK:(h + 1) * DK].astype(F32) * (scale * jnp.exp(last - col))).astype(BF16)
            add = lax.dot_general(
                u, v_v[rb, h * DV:(h + 1) * DV], (((0,), (0,)), ((), ())),
                preferred_element_type=F32,
            )
            upd[b, h] = add
            inc[h] = inc[h] * jnp.exp(last) + add

    lend[...] = inc[...].astype(BF16)

    @pl.loop(1, E)
    def _(d):
        @pl.when(ep + d < E)
        def _():
            t_copy(d).start()
            s_copy(d).start()

    @pl.loop(1, 2 * G - 1)
    def _(i):
        g, there = group_at(i)

        @pl.when(there)
        def _():
            m_copy(g, 0).wait_recv()
            z_copy(g, 0).wait_recv()
            for way in (0, 1):
                @pl.when(z_sends(g, way))
                def _():
                    m_copy(g, way).start()
                    z_copy(g, way).start()
            dispatch(g)

    for da in range(1, A):
        o1_copy(da, shard(da)).wait_recv()
        for dy in range(1, R):
            o2_copy(da, dy, yi).start()
    for db in range(1, B):
        o3_copy(0, db, tp).start()

    loads[3].wait()
    loads[4].wait()
    loads[5].wait()
    hid = (silu(dot(xz[zi], wg_v[...])) * dot(xz[zi], wu_v[...])).astype(BF16)
    shr[...] = dot(hid, wd_v[...])
    for c in loads[8:]:
        c.start()

    inc[...] = jnp.zeros_like(inc)

    @pl.loop(1, E)
    def _(i):
        d = E - i

        @pl.when(ep >= d)
        def _():
            t_copy(d).wait_recv()
            s_copy(d).wait_recv()
            for h in range(H):
                shrink = jnp.exp(trcv[d, h:h + 1, 0:1])
                inc[h] = inc[h] * shrink + srcv[d - 1, h].astype(F32)

    @pl.loop(0, nb)
    def _(b):
        crow = cum_ref[b]
        for h in range(H):
            s = inc[h]
            sblk[b, h] = s.astype(BF16)
            inc[h] = s * jnp.exp(crow[h:h + 1, BLOCK - 1:BLOCK]) + upd[b, h]

    loads[6].wait()
    loads[7].wait()
    causal = lax.broadcasted_iota(jnp.int32, (BLOCK, BLOCK), 0) >= lax.broadcasted_iota(
        jnp.int32, (BLOCK, BLOCK), 1
    )

    def retain(i):
        chunk = (tp + i) % T

        @pl.loop(0, nbc)
        def _(w):
            b = chunk * nbc + w
            rb = pl.ds(pl.multiple_of(b * BLOCK, BLOCK), BLOCK)
            ro = pl.ds(pl.multiple_of(w * BLOCK, BLOCK), BLOCK)
            cumc = cumc_ref[b]
            crow = cum_ref[b]
            for h in range(H):
                col = cumc[:, h:h + 1]
                row = crow[h:h + 1, :]
                qb = q_v[rb, h * DK:(h + 1) * DK]
                kb = k_v[rb, h * DK:(h + 1) * DK]
                vb = v_v[rb, h * DV:(h + 1) * DV]
                sc = lax.dot_general(qb, kb, (((1,), (1,)), ((), ())), preferred_element_type=F32)
                dec = jnp.exp(jnp.where(causal, col - row, 0.0))
                wt = jnp.where(causal, sc * scale * dec, 0.0).astype(BF16)
                raw = dot(wt, vb) + dot(qb, sblk[b, h]) * jnp.exp(col)
                avg = jnp.mean(raw, axis=-1, keepdims=True)
                cen = raw - avg
                var = jnp.mean(cen * cen, axis=-1, keepdims=True)
                gate = g_v[rb, h * DV:(h + 1) * DV].astype(F32)
                rs[i, ro, h * DV:(h + 1) * DV] = (
                    silu(gate) * (cen * lax.rsqrt(var + EPS))
                ).astype(BF16)

    @pl.loop(1, T)
    def _(i):
        retain(i)

    retain(0)

    loads[8].wait()
    loads[9].wait()
    loads[10].wait()

    def serve(r):
        @pl.loop(1, Pn)
        def _(d):
            d_copy(r, d).wait_recv()

        rows_in = rcv[r]
        hidden = (silu(dot(rows_in, wg_v[...])) * dot(rows_in, wu_v[...])).astype(BF16)
        res = dot(hidden, wd_v[...]).astype(BF16)
        rcv[r] = res
        ret[r, 0:C] = res[0:C]

        @pl.loop(1, Pn)
        def _(d):
            b_copy(r, d).start()

    @pl.loop(0, 2 * G - 1)
    def _(i):
        g, there = group_at(i)

        @pl.when(there)
        def _():
            serve(g)

    @pl.loop(1, T)
    def _(i):
        r_copy(i).start()

    for da in range(1, A):
        for dy in range(1, R):
            o2_copy(da, dy, (yi + R - dy) % R).wait_recv()
        for db in range(1, B):
            o3_copy(da, db, shard(da)).start()

    def combine(r):
        @pl.loop(1, Pn)
        def _(d):
            b_copy(r, d).wait_recv()

        @pl.loop(1, Pn)
        def _(d):
            d_copy(r, d).wait_send()

        dsp[r, 0:tok] = dot(dwt[r], ret[r]).astype(BF16)
        p_copy(r).start()

    @pl.loop(1, 2 * G - 1)
    def _(i):
        g, there = group_at(i)

        @pl.when(there)
        def _():
            combine(g)

    for da in range(A):
        for db in range(1, B):
            o3_copy(da, db, shard(da, db)).wait_recv()

    @pl.loop(1, T)
    def _(i):
        r_copy(i).wait_recv()

    n_col = 512
    @pl.loop(0, width // n_col)
    def _(n):
        cols = pl.ds(pl.multiple_of(n * n_col, n_col), n_col)
        acc = dot(rs[0], op_v[tp, :, cols])
        for i in range(1, T):
            acc += dot(rr[i - 1], op_v[(tp + T - i) % T, :, cols])
        mix_ref[:, cols] = acc.astype(BF16)

    @pl.loop(1, Pn)
    def _(d):
        b_copy(zi, d).wait_recv()

    shr[...] += dot(dwt[zi], ret[zi])

    @pl.loop(1, G)
    def _(i):
        g = (zi + i) % G
        p_arrival(g).wait_recv()
        shr[...] += prcv[g].astype(F32)

    moe_ref[...] = shr[...].astype(BF16)

    @pl.loop(0, G)
    def _(g):
        for way in (0, 1):
            @pl.when(z_sends(g, way))
            def _():
                m_copy(g, way).wait_send()
                z_copy(g, way).wait_send()

        @pl.when(g != zi)
        def _():
            p_copy(g).wait_send()

    @pl.loop(0, G)
    def _(r):
        @pl.loop(1, Pn)
        def _(d):
            b_copy(r, d).wait_send()

    @pl.loop(1, Pn)
    def _(d):
        d_copy(zi, d).wait_send()

    @pl.loop(1, E)
    def _(d):
        @pl.when(ep + d < E)
        def _():
            t_copy(d).wait_send()
            s_copy(d).wait_send()

    @pl.loop(1, T)
    def _(i):
        r_copy(i).wait_send()

    for da in range(A):
        if da:
            o1_copy(da, tp).wait_send()
            for dy in range(1, R):
                o2_copy(da, dy, yi).wait_send()
        for db in range(1, B):
            o3_copy(da, db, shard(da)).wait_send()


def local(
    query_rows, key_rows, value_rows, gate_rows, log_decay, out_proj,
    moe_input, norm_gain, routing, route_weight,
    expert_gate, expert_up, expert_down, shared_gate, shared_up, shared_down,
):
    E, T = lax.axis_size("ep"), lax.axis_size("tp")
    G = math.gcd(E, Z_GROUPS)
    Pn = (E // G) * T
    n = query_rows.shape[0]
    H = query_rows.shape[1] // DK
    nb = n // BLOCK
    tok, width = moe_input.shape
    visits = routing.shape[1]
    C = 2 * tok * visits // (E * T)
    ff = expert_gate.shape[2]
    assert shared_gate.shape[1] == ff
    rows_o = n // T
    dvl = H * DV

    cum = jnp.cumsum(log_decay.reshape(H, nb, BLOCK), axis=2)
    tot = jnp.sum(cum[:, :, -1], axis=1)
    tot = jnp.broadcast_to(jnp.pad(tot, (0, -H % 8))[:, None], (H + (-H % 8), 128))
    cum_b = cum.transpose(1, 0, 2)
    cum_c = cum.transpose(1, 2, 0)
    meta = jnp.concatenate([routing.T.astype(F32), route_weight.T], axis=0)

    vm = pl.BlockSpec(memory_space=pltpu.VMEM)
    hb = pl.BlockSpec(memory_space=pl.ANY)
    V = pltpu.VMEM
    dma = pltpu.SemaphoreType.DMA
    scratch = [
        V((n, H * DK), BF16), V((n, H * DK), BF16), V((n, dvl), BF16), V((n, dvl), BF16),
        V((T,) + out_proj.shape, BF16),
        V((width, ff), BF16), V((width, ff), BF16), V((ff, width), BF16),
        V((G, tok, width), BF16), V((G, 2 * visits, tok), F32),
        V((G, Pn * C, width), BF16), V((G, Pn * C, width), BF16), V((G, Pn * C, width), BF16),
        V((G, tok, Pn * C), BF16), V((tok, width), F32), V((G, tok, width), BF16),
        V((nb, H, DK, DV), F32), V((nb, H, DK, DV), BF16), V((H, DK, DV), BF16),
        V((E - 1, H, DK, DV), BF16), V((E,) + tot.shape, F32),
        V((T, rows_o, dvl), BF16), V((T - 1, rows_o, dvl), BF16), V((H, DK, DV), F32),
        dma((11,)),
        dma((2, G)), dma((G,)), dma((2, G)), dma((G,)),
        dma((G, Pn)), dma((G, Pn)), dma((G, Pn)), dma((G, Pn)),
        dma((G,)), dma((G,)),
        dma((E,)), dma((E,)), dma((E,)), dma((E,)),
        dma((T,)), dma((T,)), dma((T, E)), dma((T, E)), dma((T, T)), dma((T, T)),
        dma((T,)), dma((T,)),
    ]
    return pl.pallas_call(
        functools.partial(kernel, E, T, G, C),
        out_shape=(
            jax.ShapeDtypeStruct((rows_o, width), BF16),
            jax.ShapeDtypeStruct((tok, width), BF16),
        ),
        in_specs=[vm] * 6 + [hb] * 11,
        out_specs=(vm, vm),
        scratch_shapes=scratch,
        compiler_params=pltpu.CompilerParams(
            collective_id=0, has_side_effects=True, vmem_limit_bytes=67043328
        ),
        name="fused",
    )(
        moe_input, norm_gain[None, :], meta, cum_b, cum_c, tot,
        query_rows, key_rows, value_rows, gate_rows, out_proj,
        expert_gate, expert_up, expert_down, shared_gate, shared_up, shared_down,
    )


def solution(mesh):
    both = P(("ep", "tp"), None)
    in_specs = (
        P("ep", "tp"), P("ep", "tp"), P("ep", "tp"), P("ep", "tp"), P("tp", "ep"), P("tp", None),
        both, P(), both, both,
        P(("ep", "tp"), None, None), P(("ep", "tp"), None, None), P(("ep", "tp"), None, None),
        P(), P(), P(),
    )
    return jax.shard_map(
        local, mesh=mesh, in_specs=in_specs, out_specs=(both, both), check_vma=False
    )
```

```python
import functools
import math

import jax
import jax.numpy as jnp
from jax import lax
from jax.experimental import pallas as pl
from jax.experimental.pallas import tpu as pltpu
from jax.sharding import PartitionSpec as P

DK = 128
DV = 256
BLOCK = 128
EPS = 1e-06
Z_GROUPS = 4

F32 = jnp.float32
BF16 = jnp.bfloat16
MESH = pl.DeviceIdType.MESH


def dot(a, b):
    return jnp.dot(a, b, preferred_element_type=F32)


def silu(v):
    return v / (1.0 + jnp.exp(-v))


def kernel(
    E, T, G, C,
    x_ref, gain_ref, meta_ref, cum_ref, cumc_ref, tot_ref,
    q_hbm, k_hbm, v_hbm, g_hbm, op_hbm,
    wg_hbm, wu_hbm, wd_hbm, sg_hbm, su_hbm, sd_hbm,
    mix_ref, moe_ref,
    q_v, k_v, v_v, g_v, op_v, wg_v, wu_v, wd_v,
    xz, mz, dsp, rcv, ret, dwt, shr, prcv,
    upd, sblk, lend, srcv, trcv, rs, rr, inc,
    load_sem,
    z_s, z_r, m_s, m_r, d_s, d_r, b_s, b_r, p_s, p_r, s_s, s_r, t_s, t_r,
    o1_s, o1_r, o2_s, o2_r, o3_s, o3_r, r_s, r_r,
):
    ep = lax.axis_index("ep")
    tp = lax.axis_index("tp")
    R = E // G
    Pn = R * T
    zi = ep // R
    yi = ep % R
    j = yi * T + tp
    tok, width = x_ref.shape
    n_visits = meta_ref.shape[0] // 2
    nb = cum_ref.shape[0]
    H = cum_ref.shape[1]
    nbc = nb // T
    B = math.gcd(T, 2)
    A = T // B
    ta, tb = tp // B, tp % B
    piece = op_v.shape[1] // R
    scale = DK ** (-0.5)

    loads = [
        pltpu.make_async_copy(src, dst, load_sem.at[i])
        for i, (src, dst) in enumerate(
            ((k_hbm, k_v), (v_hbm, v_v), (op_hbm, op_v.at[tp]), (sg_hbm, wg_v), (su_hbm, wu_v),
             (sd_hbm, wd_v), (q_hbm, q_v), (g_hbm, g_v), (wg_hbm.at[0], wg_v),
             (wu_hbm.at[0], wu_v), (wd_hbm.at[0], wd_v))
        )
    ]
    for c in loads[:8]:
        c.start()

    def z_place(g):
        return (g * R + yi, tp)

    def plane_peer(d):
        p = (j + d) % Pn
        return (zi * R + p // T, p % T)

    def tp_peer(i):
        return (ep, (tp + i) % T)

    barrier = pltpu.get_barrier_semaphore()

    @pl.loop(1, Pn)
    def _(d):
        pl.semaphore_signal(barrier, inc=1, device_id=plane_peer(d), device_id_type=MESH)

    @pl.loop(1, E)
    def _(d):
        pl.semaphore_signal(barrier, inc=1, device_id=((ep + d) % E, tp), device_id_type=MESH)

    xf = x_ref[...].astype(F32)
    xz[zi] = (
        xf * lax.rsqrt(jnp.mean(xf * xf, axis=-1, keepdims=True) + EPS) * gain_ref[...]
    ).astype(BF16)
    mz[zi] = meta_ref[...]
    pl.semaphore_wait(barrier, Pn - 1 + E - 1)

    def rcopy(src, dst, ss, rs_, dev):
        return pltpu.make_async_remote_copy(
            src_ref=src, dst_ref=dst, send_sem=ss, recv_sem=rs_, device_id=dev, device_id_type=MESH
        )

    def z_copy(g, way):
        to = (zi - 1, zi + 1)[way]
        return rcopy(xz.at[g], xz.at[g], z_s.at[way, g], z_r.at[g], z_place(to))

    def m_copy(g, way):
        to = (zi - 1, zi + 1)[way]
        return rcopy(mz.at[g], mz.at[g], m_s.at[way, g], m_r.at[g], z_place(to))

    def z_sends(g, way):
        if way:
            return (g <= zi) & (zi + 1 < G)
        return (g >= zi) & (zi > 0)

    def group_at(i):
        dist = (i + 1) // 2
        g = zi + jnp.where(i % 2 == 1, -dist, dist)
        return g, (g >= 0) & (g < G)

    def rows(d):
        return pl.ds(pl.multiple_of(d * C, C), C)

    def d_copy(r, d):
        return rcopy(dsp.at[r, rows(d)], rcv.at[r, rows(d)], d_s.at[r, d], d_r.at[r, d],
                     plane_peer(d))

    def b_copy(r, d):
        return rcopy(rcv.at[r, rows(d)], ret.at[r, rows(d)], b_s.at[r, d], b_r.at[r, d],
                     plane_peer(Pn - d))

    def p_copy(g):
        return rcopy(dsp.at[g, 0:tok], prcv.at[zi], p_s.at[g], p_r.at[zi], z_place(g))

    def p_arrival(g):
        return rcopy(dsp.at[g, 0:tok], prcv.at[g], p_s.at[g], p_r.at[g], z_place(g))

    def s_copy(d):
        return rcopy(lend, srcv.at[d - 1], s_s.at[d], s_r.at[d], ((ep + d) % E, tp))

    def t_copy(d):
        return rcopy(tot_ref, trcv.at[d], t_s.at[d], t_r.at[d], ((ep + d) % E, tp))

    def shard(da, db=0):
        return ((ta + A - da) % A) * B + (tb + B - db) % B

    def part(y):
        return pl.ds(pl.multiple_of(y * piece, piece), piece)

    def o1_copy(da, src):
        at = op_v.at[src, part(yi)]
        return rcopy(at, at, o1_s.at[da], o1_r.at[da], (ep, ((ta + da) % A) * B + tb))

    def o2_copy(da, dy, y):
        at = op_v.at[shard(da), part(y)]
        return rcopy(at, at, o2_s.at[da, dy], o2_r.at[da, dy], (zi * R + (yi + dy) % R, tp))

    def o3_copy(da, db, src):
        at = op_v.at[src]
        return rcopy(at, at, o3_s.at[da, db], o3_r.at[da, db], (ep, ta * B + (tb + db) % B))

    def r_copy(i):
        return rcopy(rs.at[i], rr.at[i - 1], r_s.at[i], r_r.at[i], tp_peer(i))

    for way in (0, 1):
        @pl.when(z_sends(zi, way))
        def _():
            m_copy(zi, way).start()
            z_copy(zi, way).start()

    def dispatch(r):
        meta = mz[r]
        owner = lax.broadcasted_iota(jnp.int32, (Pn, tok), 0)
        owner = (zi * Pn + (owner + j) % Pn).astype(F32)
        member = jnp.zeros((Pn, tok), F32)
        weight = jnp.zeros((Pn, tok), F32)
        for v in range(n_visits):
            hit = meta[v:v + 1, :] == owner
            member += jnp.where(hit, 1.0, 0.0)
            weight += jnp.where(hit, meta[n_visits + v:n_visits + v + 1, :], 0.0)
        before = lax.broadcasted_iota(jnp.int32, (tok, tok), 0) < lax.broadcasted_iota(
            jnp.int32, (tok, tok), 1
        )
        rank = dot(member.astype(BF16), jnp.where(before, 1.0, 0.0).astype(BF16))
        rank = jnp.where(member > 0.5, rank, -1.0)
        slot = lax.broadcasted_iota(jnp.int32, (C, tok), 0).astype(F32)
        picks, wts = [], []
        for d in range(Pn):
            eq = slot == rank[d:d + 1, :]
            picks.append(jnp.where(eq, 1.0, 0.0))
            wts.append(jnp.where(eq, weight[d:d + 1, :], 0.0))
        pick = jnp.concatenate(picks, axis=0).astype(BF16)
        dwt[r] = jnp.concatenate(wts, axis=0).T.astype(BF16)
        out = dot(pick, xz[r]).astype(BF16)
        dsp[r] = out
        rcv[r, 0:C] = out[0:C]

        @pl.loop(1, Pn)
        def _(d):
            d_copy(r, d).start()

    dispatch(zi)

    loads[0].wait()
    loads[1].wait()

    inc[...] = jnp.zeros_like(inc)

    @pl.loop(0, nb)
    def _(b):
        rb = pl.ds(pl.multiple_of(b * BLOCK, BLOCK), BLOCK)
        cumc = cumc_ref[b]
        crow = cum_ref[b]
        for h in range(H):
            col = cumc[:, h:h + 1]
            last = crow[h:h + 1, BLOCK - 1:BLOCK]
            u = (k_v[rb, h * DK:(h + 1) * DK].astype(F32) * (scale * jnp.exp(last - col))).astype(BF16)
            add = lax.dot_general(
                u, v_v[rb, h * DV:(h + 1) * DV], (((0,), (0,)), ((), ())),
                preferred_element_type=F32,
            )
            upd[b, h] = add
            inc[h] = inc[h] * jnp.exp(last) + add

    lend[...] = inc[...].astype(BF16)

    loads[3].wait()
    loads[4].wait()
    loads[5].wait()
    hid = (silu(dot(xz[zi], wg_v[...])) * dot(xz[zi], wu_v[...])).astype(BF16)
    shr[...] = dot(hid, wd_v[...])
    for c in loads[8:]:
        c.start()

    def serve(r):
        @pl.loop(1, Pn)
        def _(d):
            d_copy(r, d).wait_recv()

        rows_in = rcv[r]
        hidden = (silu(dot(rows_in, wg_v[...])) * dot(rows_in, wu_v[...])).astype(BF16)
        res = dot(hidden, wd_v[...]).astype(BF16)
        rcv[r] = res
        ret[r, 0:C] = res[0:C]

        @pl.loop(1, Pn)
        def _(d):
            b_copy(r, d).start()

    loads[8].wait()
    loads[9].wait()
    loads[10].wait()
    @pl.loop(1, 2 * G - 1)
    def _(i):
        g, there = group_at(i)

        @pl.when(there)
        def _():
            m_copy(g, 0).wait_recv()
            z_copy(g, 0).wait_recv()
            for way in (0, 1):
                @pl.when(z_sends(g, way))
                def _():
                    m_copy(g, way).start()
                    z_copy(g, way).start()
            dispatch(g)

        behind, known = group_at(i - 2)

        @pl.when(known & (i >= 2))
        def _():
            serve(behind)

    @pl.loop(1, E)
    def _(d):
        @pl.when(ep + d < E)
        def _():
            t_copy(d).start()
            s_copy(d).start()

    loads[2].wait()
    for da in range(1, A):
        o1_copy(da, tp).start()
    for i in (2 * G - 3, 2 * G - 2):
        g, there = group_at(jnp.int32(i))

        @pl.when(there)
        def _():
            serve(g)

    inc[...] = jnp.zeros_like(inc)

    @pl.loop(1, E)
    def _(i):
        d = E - i

        @pl.when(ep >= d)
        def _():
            t_copy(d).wait_recv()
            s_copy(d).wait_recv()
            for h in range(H):
                shrink = jnp.exp(trcv[d, h:h + 1, 0:1])
                inc[h] = inc[h] * shrink + srcv[d - 1, h].astype(F32)

    @pl.loop(0, nb)
    def _(b):
        crow = cum_ref[b]
        for h in range(H):
            s = inc[h]
            sblk[b, h] = s.astype(BF16)
            inc[h] = s * jnp.exp(crow[h:h + 1, BLOCK - 1:BLOCK]) + upd[b, h]

    loads[6].wait()
    loads[7].wait()
    causal = lax.broadcasted_iota(jnp.int32, (BLOCK, BLOCK), 0) >= lax.broadcasted_iota(
        jnp.int32, (BLOCK, BLOCK), 1
    )

    def retain(i):
        chunk = (tp + i) % T

        @pl.loop(0, nbc)
        def _(w):
            b = chunk * nbc + w
            rb = pl.ds(pl.multiple_of(b * BLOCK, BLOCK), BLOCK)
            ro = pl.ds(pl.multiple_of(w * BLOCK, BLOCK), BLOCK)
            cumc = cumc_ref[b]
            crow = cum_ref[b]
            for h in range(H):
                col = cumc[:, h:h + 1]
                row = crow[h:h + 1, :]
                qb = q_v[rb, h * DK:(h + 1) * DK]
                kb = k_v[rb, h * DK:(h + 1) * DK]
                vb = v_v[rb, h * DV:(h + 1) * DV]
                sc = lax.dot_general(qb, kb, (((1,), (1,)), ((), ())), preferred_element_type=F32)
                dec = jnp.exp(jnp.where(causal, col - row, 0.0))
                wt = jnp.where(causal, sc * scale * dec, 0.0).astype(BF16)
                raw = dot(wt, vb) + dot(qb, sblk[b, h]) * jnp.exp(col)
                avg = jnp.mean(raw, axis=-1, keepdims=True)
                cen = raw - avg
                var = jnp.mean(cen * cen, axis=-1, keepdims=True)
                gate = g_v[rb, h * DV:(h + 1) * DV].astype(F32)
                rs[i, ro, h * DV:(h + 1) * DV] = (
                    silu(gate) * (cen * lax.rsqrt(var + EPS))
                ).astype(BF16)

    @pl.loop(1, T)
    def _(i):
        retain(i)

    retain(0)

    @pl.loop(1, T)
    def _(i):
        r_copy(i).start()

    for da in range(1, A):
        o1_copy(da, shard(da)).wait_recv()
        for dy in range(1, R):
            o2_copy(da, dy, yi).start()
    for db in range(1, B):
        o3_copy(0, db, tp).start()

    def combine(r):
        @pl.loop(1, Pn)
        def _(d):
            b_copy(r, d).wait_recv()

        @pl.loop(1, Pn)
        def _(d):
            d_copy(r, d).wait_send()

        dsp[r, 0:tok] = dot(dwt[r], ret[r]).astype(BF16)
        p_copy(r).start()

    @pl.loop(1, 2 * G - 1)
    def _(i):
        g, there = group_at(i)

        @pl.when(there)
        def _():
            combine(g)

    for da in range(1, A):
        for dy in range(1, R):
            o2_copy(da, dy, (yi + R - dy) % R).wait_recv()
        for db in range(1, B):
            o3_copy(da, db, shard(da)).start()

    for da in range(A):
        for db in range(1, B):
            o3_copy(da, db, shard(da, db)).wait_recv()

    @pl.loop(1, T)
    def _(i):
        r_copy(i).wait_recv()

    n_col = 512
    @pl.loop(0, width // n_col)
    def _(n):
        cols = pl.ds(pl.multiple_of(n * n_col, n_col), n_col)
        acc = dot(rs[0], op_v[tp, :, cols])
        for i in range(1, T):
            acc += dot(rr[i - 1], op_v[(tp + T - i) % T, :, cols])
        mix_ref[:, cols] = acc.astype(BF16)

    @pl.loop(1, Pn)
    def _(d):
        b_copy(zi, d).wait_recv()

    shr[...] += dot(dwt[zi], ret[zi])

    @pl.loop(1, G)
    def _(i):
        g = (zi + i) % G
        p_arrival(g).wait_recv()
        shr[...] += prcv[g].astype(F32)

    moe_ref[...] = shr[...].astype(BF16)

    @pl.loop(0, G)
    def _(g):
        for way in (0, 1):
            @pl.when(z_sends(g, way))
            def _():
                m_copy(g, way).wait_send()
                z_copy(g, way).wait_send()

        @pl.when(g != zi)
        def _():
            p_copy(g).wait_send()

    @pl.loop(0, G)
    def _(r):
        @pl.loop(1, Pn)
        def _(d):
            b_copy(r, d).wait_send()

    @pl.loop(1, Pn)
    def _(d):
        d_copy(zi, d).wait_send()

    @pl.loop(1, E)
    def _(d):
        @pl.when(ep + d < E)
        def _():
            t_copy(d).wait_send()
            s_copy(d).wait_send()

    @pl.loop(1, T)
    def _(i):
        r_copy(i).wait_send()

    for da in range(A):
        if da:
            o1_copy(da, tp).wait_send()
            for dy in range(1, R):
                o2_copy(da, dy, yi).wait_send()
        for db in range(1, B):
            o3_copy(da, db, shard(da)).wait_send()


def local(
    query_rows, key_rows, value_rows, gate_rows, log_decay, out_proj,
    moe_input, norm_gain, routing, route_weight,
    expert_gate, expert_up, expert_down, shared_gate, shared_up, shared_down,
):
    E, T = lax.axis_size("ep"), lax.axis_size("tp")
    G = math.gcd(E, Z_GROUPS)
    Pn = (E // G) * T
    n = query_rows.shape[0]
    H = query_rows.shape[1] // DK
    nb = n // BLOCK
    tok, width = moe_input.shape
    visits = routing.shape[1]
    C = 2 * tok * visits // (E * T)
    ff = expert_gate.shape[2]
    assert shared_gate.shape[1] == ff
    rows_o = n // T
    dvl = H * DV

    cum = jnp.cumsum(log_decay.reshape(H, nb, BLOCK), axis=2)
    tot = jnp.sum(cum[:, :, -1], axis=1)
    tot = jnp.broadcast_to(jnp.pad(tot, (0, -H % 8))[:, None], (H + (-H % 8), 128))
    cum_b = cum.transpose(1, 0, 2)
    cum_c = cum.transpose(1, 2, 0)
    meta = jnp.concatenate([routing.T.astype(F32), route_weight.T], axis=0)

    vm = pl.BlockSpec(memory_space=pltpu.VMEM)
    hb = pl.BlockSpec(memory_space=pl.ANY)
    V = pltpu.VMEM
    dma = pltpu.SemaphoreType.DMA
    scratch = [
        V((n, H * DK), BF16), V((n, H * DK), BF16), V((n, dvl), BF16), V((n, dvl), BF16),
        V((T,) + out_proj.shape, BF16),
        V((width, ff), BF16), V((width, ff), BF16), V((ff, width), BF16),
        V((G, tok, width), BF16), V((G, 2 * visits, tok), F32),
        V((G, Pn * C, width), BF16), V((G, Pn * C, width), BF16), V((G, Pn * C, width), BF16),
        V((G, tok, Pn * C), BF16), V((tok, width), F32), V((G, tok, width), BF16),
        V((nb, H, DK, DV), F32), V((nb, H, DK, DV), BF16), V((H, DK, DV), BF16),
        V((E - 1, H, DK, DV), BF16), V((E,) + tot.shape, F32),
        V((T, rows_o, dvl), BF16), V((T - 1, rows_o, dvl), BF16), V((H, DK, DV), F32),
        dma((11,)),
        dma((2, G)), dma((G,)), dma((2, G)), dma((G,)),
        dma((G, Pn)), dma((G, Pn)), dma((G, Pn)), dma((G, Pn)),
        dma((G,)), dma((G,)),
        dma((E,)), dma((E,)), dma((E,)), dma((E,)),
        dma((T,)), dma((T,)), dma((T, E)), dma((T, E)), dma((T, T)), dma((T, T)),
        dma((T,)), dma((T,)),
    ]
    return pl.pallas_call(
        functools.partial(kernel, E, T, G, C),
        out_shape=(
            jax.ShapeDtypeStruct((rows_o, width), BF16),
            jax.ShapeDtypeStruct((tok, width), BF16),
        ),
        in_specs=[vm] * 6 + [hb] * 11,
        out_specs=(vm, vm),
        scratch_shapes=scratch,
        compiler_params=pltpu.CompilerParams(
            collective_id=0, has_side_effects=True, vmem_limit_bytes=67043328
        ),
        name="fused",
    )(
        moe_input, norm_gain[None, :], meta, cum_b, cum_c, tot,
        query_rows, key_rows, value_rows, gate_rows, out_proj,
        expert_gate, expert_up, expert_down, shared_gate, shared_up, shared_down,
    )


def solution(mesh):
    both = P(("ep", "tp"), None)
    in_specs = (
        P("ep", "tp"), P("ep", "tp"), P("ep", "tp"), P("ep", "tp"), P("tp", "ep"), P("tp", None),
        both, P(), both, both,
        P(("ep", "tp"), None, None), P(("ep", "tp"), None, None), P(("ep", "tp"), None, None),
        P(), P(), P(),
    )
    return jax.shard_map(
        local, mesh=mesh, in_specs=in_specs, out_specs=(both, both), check_vma=False
    )
```

```python
import functools
import math

import jax
import jax.numpy as jnp
from jax import lax
from jax.experimental import pallas as pl
from jax.experimental.pallas import tpu as pltpu
from jax.sharding import PartitionSpec as P

DK = 128
DV = 256
BLOCK = 128
EPS = 1e-06
Z_GROUPS = 4

F32 = jnp.float32
BF16 = jnp.bfloat16
MESH = pl.DeviceIdType.MESH


def dot(a, b):
    return jnp.dot(a, b, preferred_element_type=F32)


def silu(v):
    return v / (1.0 + jnp.exp(-v))


def kernel(
    E, T, G, C,
    x_ref, gain_ref, meta_ref, cum_ref, cumc_ref, tot_ref,
    q_hbm, k_hbm, v_hbm, g_hbm, op_hbm,
    wg_hbm, wu_hbm, wd_hbm, sg_hbm, su_hbm, sd_hbm,
    mix_ref, moe_ref,
    q_v, k_v, v_v, g_v, op_v, wg_v, wu_v, wd_v,
    xz, mz, dsp, rcv, ret, dwt, shr, prcv,
    upd, sblk, lend, srcv, trcv, rs, rr, inc,
    load_sem,
    z_s, z_r, m_s, m_r, d_s, d_r, b_s, b_r, p_s, p_r, s_s, s_r, t_s, t_r,
    o1_s, o1_r, o2_s, o2_r, o3_s, o3_r, r_s, r_r,
):
    ep = lax.axis_index("ep")
    tp = lax.axis_index("tp")
    R = E // G
    Pn = R * T
    zi = ep // R
    yi = ep % R
    j = yi * T + tp
    tok, width = x_ref.shape
    n_visits = meta_ref.shape[0] // 2
    nb = cum_ref.shape[0]
    H = cum_ref.shape[1]
    nbc = nb // T
    B = math.gcd(T, 2)
    A = T // B
    ta, tb = tp // B, tp % B
    piece = op_v.shape[1] // R
    scale = DK ** (-0.5)

    loads = [
        pltpu.make_async_copy(src, dst, load_sem.at[i])
        for i, (src, dst) in enumerate(
            ((k_hbm, k_v), (v_hbm, v_v), (op_hbm, op_v.at[tp]), (sg_hbm, wg_v), (su_hbm, wu_v),
             (sd_hbm, wd_v), (q_hbm, q_v), (g_hbm, g_v), (wg_hbm.at[0], wg_v),
             (wu_hbm.at[0], wu_v), (wd_hbm.at[0], wd_v))
        )
    ]
    for c in loads[:8]:
        c.start()

    def z_place(g):
        return (g * R + yi, tp)

    def plane_peer(d):
        p = (j + d) % Pn
        return (zi * R + p // T, p % T)

    def tp_peer(i):
        return (ep, (tp + i) % T)

    barrier = pltpu.get_barrier_semaphore()

    @pl.loop(1, Pn)
    def _(d):
        pl.semaphore_signal(barrier, inc=1, device_id=plane_peer(d), device_id_type=MESH)

    @pl.loop(1, E)
    def _(d):
        pl.semaphore_signal(barrier, inc=1, device_id=((ep + d) % E, tp), device_id_type=MESH)

    xf = x_ref[...].astype(F32)
    xz[zi] = (
        xf * lax.rsqrt(jnp.mean(xf * xf, axis=-1, keepdims=True) + EPS) * gain_ref[...]
    ).astype(BF16)
    mz[zi] = meta_ref[...]
    pl.semaphore_wait(barrier, Pn - 1 + E - 1)

    def rcopy(src, dst, ss, rs_, dev):
        return pltpu.make_async_remote_copy(
            src_ref=src, dst_ref=dst, send_sem=ss, recv_sem=rs_, device_id=dev, device_id_type=MESH
        )

    def z_copy(g, way):
        to = (zi - 1, zi + 1)[way]
        return rcopy(xz.at[g], xz.at[g], z_s.at[way, g], z_r.at[g], z_place(to))

    def m_copy(g, way):
        to = (zi - 1, zi + 1)[way]
        return rcopy(mz.at[g], mz.at[g], m_s.at[way, g], m_r.at[g], z_place(to))

    def z_sends(g, way):
        if way:
            return (g <= zi) & (zi + 1 < G)
        return (g >= zi) & (zi > 0)

    def group_at(i):
        dist = (i + 1) // 2
        g = zi + jnp.where(i % 2 == 1, -dist, dist)
        return g, (g >= 0) & (g < G)

    def rows(d):
        return pl.ds(pl.multiple_of(d * C, C), C)

    def d_copy(r, d):
        return rcopy(dsp.at[r, rows(d)], rcv.at[r, rows(d)], d_s.at[r, d], d_r.at[r, d],
                     plane_peer(d))

    def b_copy(r, d):
        return rcopy(rcv.at[r, rows(d)], ret.at[r, rows(d)], b_s.at[r, d], b_r.at[r, d],
                     plane_peer(Pn - d))

    def p_copy(g):
        return rcopy(dsp.at[g, 0:tok], prcv.at[zi], p_s.at[g], p_r.at[zi], z_place(g))

    def p_arrival(g):
        return rcopy(dsp.at[g, 0:tok], prcv.at[g], p_s.at[g], p_r.at[g], z_place(g))

    def s_copy(d):
        return rcopy(lend, srcv.at[d - 1], s_s.at[d], s_r.at[d], ((ep + d) % E, tp))

    def t_copy(d):
        return rcopy(tot_ref, trcv.at[d], t_s.at[d], t_r.at[d], ((ep + d) % E, tp))

    def shard(da, db=0):
        return ((ta + A - da) % A) * B + (tb + B - db) % B

    def part(y):
        return pl.ds(pl.multiple_of(y * piece, piece), piece)

    def o1_copy(da, src):
        at = op_v.at[src, part(yi)]
        return rcopy(at, at, o1_s.at[da], o1_r.at[da], (ep, ((ta + da) % A) * B + tb))

    def o2_copy(da, dy, y):
        at = op_v.at[shard(da), part(y)]
        return rcopy(at, at, o2_s.at[da, dy], o2_r.at[da, dy], (zi * R + (yi + dy) % R, tp))

    def o3_copy(da, db, src):
        at = op_v.at[src]
        return rcopy(at, at, o3_s.at[da, db], o3_r.at[da, db], (ep, ta * B + (tb + db) % B))

    def r_copy(i):
        return rcopy(rs.at[i], rr.at[i - 1], r_s.at[i], r_r.at[i], tp_peer(i))

    for way in (0, 1):
        @pl.when(z_sends(zi, way))
        def _():
            m_copy(zi, way).start()
            z_copy(zi, way).start()

    def dispatch(r):
        meta = mz[r]
        owner = lax.broadcasted_iota(jnp.int32, (Pn, tok), 0)
        owner = (zi * Pn + (owner + j) % Pn).astype(F32)
        member = jnp.zeros((Pn, tok), F32)
        weight = jnp.zeros((Pn, tok), F32)
        for v in range(n_visits):
            hit = meta[v:v + 1, :] == owner
            member += jnp.where(hit, 1.0, 0.0)
            weight += jnp.where(hit, meta[n_visits + v:n_visits + v + 1, :], 0.0)
        before = lax.broadcasted_iota(jnp.int32, (tok, tok), 0) < lax.broadcasted_iota(
            jnp.int32, (tok, tok), 1
        )
        rank = dot(member.astype(BF16), jnp.where(before, 1.0, 0.0).astype(BF16))
        rank = jnp.where(member > 0.5, rank, -1.0)
        slot = lax.broadcasted_iota(jnp.int32, (C, tok), 0).astype(F32)
        picks, wts = [], []
        for d in range(Pn):
            eq = slot == rank[d:d + 1, :]
            picks.append(jnp.where(eq, 1.0, 0.0))
            wts.append(jnp.where(eq, weight[d:d + 1, :], 0.0))
        pick = jnp.concatenate(picks, axis=0).astype(BF16)
        dwt[r] = jnp.concatenate(wts, axis=0).T.astype(BF16)
        out = dot(pick, xz[r]).astype(BF16)
        dsp[r] = out
        rcv[r, 0:C] = out[0:C]

        @pl.loop(1, Pn)
        def _(d):
            d_copy(r, d).start()

    dispatch(zi)

    loads[0].wait()
    loads[1].wait()

    inc[...] = jnp.zeros_like(inc)

    @pl.loop(0, nb)
    def _(b):
        rb = pl.ds(pl.multiple_of(b * BLOCK, BLOCK), BLOCK)
        cumc = cumc_ref[b]
        crow = cum_ref[b]
        for h in range(H):
            col = cumc[:, h:h + 1]
            last = crow[h:h + 1, BLOCK - 1:BLOCK]
            u = (k_v[rb, h * DK:(h + 1) * DK].astype(F32) * (scale * jnp.exp(last - col))).astype(BF16)
            add = lax.dot_general(
                u, v_v[rb, h * DV:(h + 1) * DV], (((0,), (0,)), ((), ())),
                preferred_element_type=F32,
            )
            upd[b, h] = add
            inc[h] = inc[h] * jnp.exp(last) + add

    lend[...] = inc[...].astype(BF16)

    loads[3].wait()
    loads[4].wait()
    loads[5].wait()
    hid = (silu(dot(xz[zi], wg_v[...])) * dot(xz[zi], wu_v[...])).astype(BF16)
    shr[...] = dot(hid, wd_v[...])
    for c in loads[8:]:
        c.start()

    def serve(r):
        @pl.loop(1, Pn)
        def _(d):
            d_copy(r, d).wait_recv()

        rows_in = rcv[r]
        hidden = (silu(dot(rows_in, wg_v[...])) * dot(rows_in, wu_v[...])).astype(BF16)
        res = dot(hidden, wd_v[...]).astype(BF16)
        rcv[r] = res
        ret[r, 0:C] = res[0:C]

        @pl.loop(1, Pn)
        def _(d):
            b_copy(r, d).start()

    loads[8].wait()
    loads[9].wait()
    loads[10].wait()
    @pl.loop(1, 2 * G - 1)
    def _(i):
        g, there = group_at(i)

        @pl.when(there)
        def _():
            m_copy(g, 0).wait_recv()
            z_copy(g, 0).wait_recv()
            for way in (0, 1):
                @pl.when(z_sends(g, way))
                def _():
                    m_copy(g, way).start()
                    z_copy(g, way).start()
            dispatch(g)

        @pl.when(i == G - 1)
        def _():
            @pl.loop(1, E)
            def _(d):
                @pl.when(ep + d < E)
                def _():
                    t_copy(d).start()
                    s_copy(d).start()

        behind, known = group_at(i - 2)

        @pl.when(known & (i >= 2))
        def _():
            serve(behind)

    loads[2].wait()
    for da in range(1, A):
        o1_copy(da, tp).start()
    for i in (2 * G - 3, 2 * G - 2):
        g, there = group_at(jnp.int32(i))

        @pl.when(there)
        def _():
            serve(g)

    inc[...] = jnp.zeros_like(inc)

    @pl.loop(1, E)
    def _(i):
        d = E - i

        @pl.when(ep >= d)
        def _():
            t_copy(d).wait_recv()
            s_copy(d).wait_recv()
            for h in range(H):
                shrink = jnp.exp(trcv[d, h:h + 1, 0:1])
                inc[h] = inc[h] * shrink + srcv[d - 1, h].astype(F32)

    @pl.loop(0, nb)
    def _(b):
        crow = cum_ref[b]
        for h in range(H):
            s = inc[h]
            sblk[b, h] = s.astype(BF16)
            inc[h] = s * jnp.exp(crow[h:h + 1, BLOCK - 1:BLOCK]) + upd[b, h]

    loads[6].wait()
    loads[7].wait()
    causal = lax.broadcasted_iota(jnp.int32, (BLOCK, BLOCK), 0) >= lax.broadcasted_iota(
        jnp.int32, (BLOCK, BLOCK), 1
    )

    def retain(i):
        chunk = (tp + i) % T

        @pl.loop(0, nbc)
        def _(w):
            b = chunk * nbc + w
            rb = pl.ds(pl.multiple_of(b * BLOCK, BLOCK), BLOCK)
            ro = pl.ds(pl.multiple_of(w * BLOCK, BLOCK), BLOCK)
            cumc = cumc_ref[b]
            crow = cum_ref[b]
            for h in range(H):
                col = cumc[:, h:h + 1]
                row = crow[h:h + 1, :]
                qb = q_v[rb, h * DK:(h + 1) * DK]
                kb = k_v[rb, h * DK:(h + 1) * DK]
                vb = v_v[rb, h * DV:(h + 1) * DV]
                sc = lax.dot_general(qb, kb, (((1,), (1,)), ((), ())), preferred_element_type=F32)
                dec = jnp.exp(jnp.where(causal, col - row, 0.0))
                wt = jnp.where(causal, sc * scale * dec, 0.0).astype(BF16)
                raw = dot(wt, vb) + dot(qb, sblk[b, h]) * jnp.exp(col)
                avg = jnp.mean(raw, axis=-1, keepdims=True)
                cen = raw - avg
                var = jnp.mean(cen * cen, axis=-1, keepdims=True)
                gate = g_v[rb, h * DV:(h + 1) * DV].astype(F32)
                rs[i, ro, h * DV:(h + 1) * DV] = (
                    silu(gate) * (cen * lax.rsqrt(var + EPS))
                ).astype(BF16)

    @pl.loop(1, T)
    def _(i):
        retain(i)

    retain(0)

    @pl.loop(1, T)
    def _(i):
        r_copy(i).start()

    def combine(r):
        @pl.loop(1, Pn)
        def _(d):
            b_copy(r, d).wait_recv()

        @pl.loop(1, Pn)
        def _(d):
            d_copy(r, d).wait_send()

        dsp[r, 0:tok] = dot(dwt[r], ret[r]).astype(BF16)
        p_copy(r).start()

    @pl.loop(1, 2 * G - 1)
    def _(i):
        g, there = group_at(i)

        @pl.when(there)
        def _():
            combine(g)

    for da in range(1, A):
        o1_copy(da, shard(da)).wait_recv()
        for dy in range(1, R):
            o2_copy(da, dy, yi).start()
    for db in range(1, B):
        o3_copy(0, db, tp).start()

    for da in range(1, A):
        for dy in range(1, R):
            o2_copy(da, dy, (yi + R - dy) % R).wait_recv()
        for db in range(1, B):
            o3_copy(da, db, shard(da)).start()

    for da in range(A):
        for db in range(1, B):
            o3_copy(da, db, shard(da, db)).wait_recv()

    @pl.loop(1, T)
    def _(i):
        r_copy(i).wait_recv()

    n_col = 512
    @pl.loop(0, width // n_col)
    def _(n):
        cols = pl.ds(pl.multiple_of(n * n_col, n_col), n_col)
        acc = dot(rs[0], op_v[tp, :, cols])
        for i in range(1, T):
            acc += dot(rr[i - 1], op_v[(tp + T - i) % T, :, cols])
        mix_ref[:, cols] = acc.astype(BF16)

    @pl.loop(1, Pn)
    def _(d):
        b_copy(zi, d).wait_recv()

    shr[...] += dot(dwt[zi], ret[zi])

    @pl.loop(1, G)
    def _(i):
        g = (zi + i) % G
        p_arrival(g).wait_recv()
        shr[...] += prcv[g].astype(F32)

    moe_ref[...] = shr[...].astype(BF16)

    @pl.loop(0, G)
    def _(g):
        for way in (0, 1):
            @pl.when(z_sends(g, way))
            def _():
                m_copy(g, way).wait_send()
                z_copy(g, way).wait_send()

        @pl.when(g != zi)
        def _():
            p_copy(g).wait_send()

    @pl.loop(0, G)
    def _(r):
        @pl.loop(1, Pn)
        def _(d):
            b_copy(r, d).wait_send()

    @pl.loop(1, Pn)
    def _(d):
        d_copy(zi, d).wait_send()

    @pl.loop(1, E)
    def _(d):
        @pl.when(ep + d < E)
        def _():
            t_copy(d).wait_send()
            s_copy(d).wait_send()

    @pl.loop(1, T)
    def _(i):
        r_copy(i).wait_send()

    for da in range(A):
        if da:
            o1_copy(da, tp).wait_send()
            for dy in range(1, R):
                o2_copy(da, dy, yi).wait_send()
        for db in range(1, B):
            o3_copy(da, db, shard(da)).wait_send()


def local(
    query_rows, key_rows, value_rows, gate_rows, log_decay, out_proj,
    moe_input, norm_gain, routing, route_weight,
    expert_gate, expert_up, expert_down, shared_gate, shared_up, shared_down,
):
    E, T = lax.axis_size("ep"), lax.axis_size("tp")
    G = math.gcd(E, Z_GROUPS)
    Pn = (E // G) * T
    n = query_rows.shape[0]
    H = query_rows.shape[1] // DK
    nb = n // BLOCK
    tok, width = moe_input.shape
    visits = routing.shape[1]
    C = 2 * tok * visits // (E * T)
    ff = expert_gate.shape[2]
    assert shared_gate.shape[1] == ff
    rows_o = n // T
    dvl = H * DV

    cum = jnp.cumsum(log_decay.reshape(H, nb, BLOCK), axis=2)
    tot = jnp.sum(cum[:, :, -1], axis=1)
    tot = jnp.broadcast_to(jnp.pad(tot, (0, -H % 8))[:, None], (H + (-H % 8), 128))
    cum_b = cum.transpose(1, 0, 2)
    cum_c = cum.transpose(1, 2, 0)
    meta = jnp.concatenate([routing.T.astype(F32), route_weight.T], axis=0)

    vm = pl.BlockSpec(memory_space=pltpu.VMEM)
    hb = pl.BlockSpec(memory_space=pl.ANY)
    V = pltpu.VMEM
    dma = pltpu.SemaphoreType.DMA
    scratch = [
        V((n, H * DK), BF16), V((n, H * DK), BF16), V((n, dvl), BF16), V((n, dvl), BF16),
        V((T,) + out_proj.shape, BF16),
        V((width, ff), BF16), V((width, ff), BF16), V((ff, width), BF16),
        V((G, tok, width), BF16), V((G, 2 * visits, tok), F32),
        V((G, Pn * C, width), BF16), V((G, Pn * C, width), BF16), V((G, Pn * C, width), BF16),
        V((G, tok, Pn * C), BF16), V((tok, width), F32), V((G, tok, width), BF16),
        V((nb, H, DK, DV), F32), V((nb, H, DK, DV), BF16), V((H, DK, DV), BF16),
        V((E - 1, H, DK, DV), BF16), V((E,) + tot.shape, F32),
        V((T, rows_o, dvl), BF16), V((T - 1, rows_o, dvl), BF16), V((H, DK, DV), F32),
        dma((11,)),
        dma((2, G)), dma((G,)), dma((2, G)), dma((G,)),
        dma((G, Pn)), dma((G, Pn)), dma((G, Pn)), dma((G, Pn)),
        dma((G,)), dma((G,)),
        dma((E,)), dma((E,)), dma((E,)), dma((E,)),
        dma((T,)), dma((T,)), dma((T, E)), dma((T, E)), dma((T, T)), dma((T, T)),
        dma((T,)), dma((T,)),
    ]
    return pl.pallas_call(
        functools.partial(kernel, E, T, G, C),
        out_shape=(
            jax.ShapeDtypeStruct((rows_o, width), BF16),
            jax.ShapeDtypeStruct((tok, width), BF16),
        ),
        in_specs=[vm] * 6 + [hb] * 11,
        out_specs=(vm, vm),
        scratch_shapes=scratch,
        compiler_params=pltpu.CompilerParams(
            collective_id=0, has_side_effects=True, vmem_limit_bytes=67043328
        ),
        name="fused",
    )(
        moe_input, norm_gain[None, :], meta, cum_b, cum_c, tot,
        query_rows, key_rows, value_rows, gate_rows, out_proj,
        expert_gate, expert_up, expert_down, shared_gate, shared_up, shared_down,
    )


def solution(mesh):
    both = P(("ep", "tp"), None)
    in_specs = (
        P("ep", "tp"), P("ep", "tp"), P("ep", "tp"), P("ep", "tp"), P("tp", "ep"), P("tp", None),
        both, P(), both, both,
        P(("ep", "tp"), None, None), P(("ep", "tp"), None, None), P(("ep", "tp"), None, None),
        P(), P(), P(),
    )
    return jax.shard_map(
        local, mesh=mesh, in_specs=in_specs, out_specs=(both, both), check_vma=False
    )
```
